32 devices in a mesh: gr: 2 (over x), fs: 4 (over z), tp: 4 (over y, core).
Axes of the slice: x: 2, y: 2, z: 4, core: 2. Of those that a mesh axis runs over, the one named last changes fastest.
Arguments:
- tokens: bfloat16 [4096, 2048], P(('gr', 'fs', 'tp')), may hold values from -6 to 6
- norm_gain: float32 [2048], P('fs'), may hold values from 0.1 to 1.9
- gate_master: float32 [16, 2048, 256], P(None, 'fs', ('gr', 'tp')), may hold values from -0.125 to 0.125
- up_master: float32 [16, 2048, 256], P(None, 'fs', ('gr', 'tp')), may hold values from -0.125 to 0.125
- down_master: float32 [16, 256, 2048], P(None, 'fs', ('gr', 'tp')), may hold values from -0.375 to 0.375
- route_group: int32 [4096], P(('gr', 'fs', 'tp')), may hold values from 0 to 3
- route_expert: int32 [4096, 2], P(('gr', 'fs', 'tp')), may hold values from 0 to 3, all different within a row
- route_weight: float32 [4096, 2], P(('gr', 'fs', 'tp')), may hold values from 0.1 to 1
Outputs:
- gate_new: bfloat16 [16, 2048, 256], P(('fs', 'tp'))
- up_new: bfloat16 [16, 2048, 256], P(('fs', 'tp'))
- down_new: bfloat16 [16, 256, 2048], P(('fs', 'tp'))
- mixed: bfloat16 [4096, 2048], P(('gr', 'fs', 'tp'))
The draws below stay inside these ranges and needn't reach their ends.
Inputs may be any that keep to these rules, and one draw needn't show every extreme that they name: `route_expert`: the 2 entries of a row are different.
All inputs are finite; a program needn't handle non-finite values.
Results may differ from the reference program's by a relative error of at most 0.0086.
Values may be sent and summed in bfloat16 or wider, within the bound.
A program may use at most 64 MiB of HBM per device.

```python
import math
import jax
import jax.numpy as jnp
from jax import lax

D = 2048
F = 256
E_GROUPS = 4
TOP = 2
TOK_DEV = 128
EXPERTS = 16
EPG = 4
TOKENS = 4096
CAP = 24


def touch_ends(drawn, stream_key, smallest, top_value):
    place = [jax.random.randint(jax.random.fold_in(stream_key, axis), (), 0, length) for axis, length in enumerate(drawn.shape)]
    longest = drawn.shape.index(max(drawn.shape))
    next_to = place[:longest] + [(place[longest] + 1) % drawn.shape[longest]] + place[longest + 1:]
    return drawn.at[tuple(place)].set(smallest).at[tuple(next_to)].set(top_value)


def steps_of(rng, dims, cuts, low, high):
    loudness, own = 1.0, jax.random.fold_in(rng, 6)
    for dim, blocks in cuts:
        steps = jnp.exp(jax.random.uniform(jax.random.fold_in(own, dim), (blocks,), jnp.float32, low / len(cuts), high / len(cuts)))
        loudness = loudness * jnp.repeat(steps, dims[dim] // blocks).reshape([-1 if axis == dim else 1 for axis in range(len(dims))])
    return loudness


def choose_distinct(key, rows, number_of, top, lift):
    order = jax.random.permutation(jax.random.fold_in(key, 1), number_of)
    pull = order
    for power in range(3):
        pull = pull * pull // number_of
    pull = pull * lift // number_of
    tickets = jax.random.randint(jax.random.fold_in(key, 2), (rows, number_of), 0, 4096) + pull
    fixed_rows = jax.random.permutation(jax.random.fold_in(key, 3), rows)[jnp.arange(number_of) % rows]
    tickets = jnp.where(jnp.arange(rows)[:, None] == fixed_rows[None, :], 1 << 14, tickets)
    priority = tickets * number_of + jnp.arange(number_of)
    return lax.top_k(priority.astype(jnp.int32), top)[1].astype(jnp.int32)


def scatter_about(key, shape, scale, most, shards=(), held_as=jnp.bfloat16):
    gain = steps_of(key, shape, shards, -0.22, 0.18) if shards else 1.0
    result = jax.random.normal(key, shape, jnp.float32) * scale * gain
    return jnp.minimum(jnp.maximum(result, -most), most).astype(held_as)


def setup_inputs(seed: int = 0) -> dict:
    seeds = jax.random.split(jax.random.key(seed), 9)
    return {
        "tokens": scatter_about(seeds[0], (TOKENS, D), 1.0, 6.0, ((0, 32),)),
        "norm_gain": jnp.clip(1.0 + 0.18 * jax.random.normal(seeds[1], (D,), jnp.float32), 0.1, 1.9),
        "gate_master": scatter_about(seeds[2], (EXPERTS, D, F), D ** -0.5, 0.125, ((1, 4), (2, 8)), jnp.float32),
        "up_master": scatter_about(seeds[3], (EXPERTS, D, F), D ** -0.5, 0.125, ((1, 4), (2, 8)), jnp.float32),
        "down_master": scatter_about(seeds[4], (EXPERTS, F, D), F ** -0.5, 0.375, ((1, 4), (2, 8)), jnp.float32),
        "route_group": touch_ends(jax.random.randint(seeds[5], (TOKENS,), 0, E_GROUPS), jax.random.fold_in(seeds[5], 1), 0, E_GROUPS - 1).astype(jnp.int32),
        "route_expert": choose_distinct(seeds[6], TOKENS, EPG, TOP, 4096),
        "route_weight": jnp.clip(jnp.exp(math.log(1.0) - 2.3025851 * jax.random.uniform(seeds[7], (TOKENS, TOP), jnp.float32) ** steps_of(seeds[7], (TOKENS, TOP), ((0, 32),), -0.2, 0.2)), 0.1, 1.0),
    }


def reference(tokens, norm_gain, gate_master, up_master, down_master, route_group, route_expert, route_weight):
    gate_new = (gate_master * norm_gain[None, :, None]).astype(jnp.bfloat16)
    up_new = (up_master * norm_gain[None, :, None]).astype(jnp.bfloat16)
    down_new = down_master.astype(jnp.bfloat16)
    floats = tokens.astype(jnp.float32)
    normed = (floats * lax.rsqrt(lax.optimization_barrier(jnp.mean(floats * floats, axis=-1, keepdims=True)) + 1e-06)).astype(jnp.bfloat16)
    sources = TOKENS // TOK_DEV
    expert_id = (route_group[:, None] * EPG + route_expert).astype(jnp.int32)
    blocks = expert_id.reshape(sources, TOK_DEV * TOP)
    columns = jnp.arange(EXPERTS).astype(jnp.int32)
    onehot = (blocks[:, :, None] == columns[None, None, :]).astype(jnp.int32)
    rank = lax.optimization_barrier(jnp.sum((jnp.cumsum(onehot, axis=1) - 1) * onehot, axis=2)).astype(jnp.int32)
    source_ids = jnp.arange(sources).astype(jnp.int32)[:, None]
    dump = EXPERTS * sources * CAP
    slot = jnp.where(rank < CAP, blocks * (sources * CAP) + source_ids * CAP + rank, dump).reshape(-1).astype(jnp.int32)
    rows = jnp.repeat(normed, TOP, axis=0)
    buffer = jnp.zeros((dump + 1, D), jnp.bfloat16).at[slot].set(rows)[:-1].reshape(EXPERTS, sources * CAP, D)

    def expert(operands):
        block, w_gate, w_up, w_down = operands
        gate = jnp.dot(block, w_gate, preferred_element_type=jnp.float32)
        upper = jnp.dot(block, w_up, preferred_element_type=jnp.float32)
        hidden = (jax.nn.silu(gate) * upper).astype(jnp.bfloat16)
        return jnp.dot(hidden, w_down, preferred_element_type=jnp.float32).astype(jnp.bfloat16)
    outcome = lax.map(expert, (buffer, gate_new, up_new, down_new))
    table = jnp.concatenate([outcome.reshape(-1, D), jnp.zeros((1, D), jnp.bfloat16)], axis=0)
    picked = table[slot].reshape(TOKENS, TOP, D).astype(jnp.float32)
    mixed = lax.optimization_barrier(jnp.sum(picked * route_weight[:, :, None], axis=1)).astype(jnp.bfloat16)
    return (gate_new, up_new, down_new, mixed)
```

```python
import functools

import jax
import jax.numpy as jnp
from jax import lax
from jax.experimental import pallas as pl
from jax.experimental.pallas import tpu as pltpu
from jax.sharding import PartitionSpec as P

E_GROUPS = 4
TOP = 2
MESH = pl.DeviceIdType.MESH
ANY = pl.BlockSpec(memory_space=pl.ANY)


def place(expert, n_tp):
    return {"fs": expert // n_tp, "tp": lax.rem(expert, n_tp)}


def greet(me, experts, n_tp, my_gr, n_gr):
    barrier = pltpu.get_barrier_semaphore()

    def hello(step, carry):
        pl.semaphore_signal(
            barrier,
            inc=1,
            device_id=place(lax.rem(me + step, experts), n_tp),
            device_id_type=MESH,
        )
        return carry

    lax.fori_loop(1, experts, hello, 0)
    for step in range(1, n_gr):
        pl.semaphore_signal(
            barrier, inc=1, device_id={"gr": lax.rem(my_gr + step, n_gr)}, device_id_type=MESH
        )
    pl.semaphore_wait(barrier, experts - 1 + n_gr - 1)


def send(src, dst, send_sem, recv_sem, where):
    return pltpu.make_async_remote_copy(
        src_ref=src,
        dst_ref=dst,
        send_sem=send_sem,
        recv_sem=recv_sem,
        device_id=where,
        device_id_type=MESH,
    )


def wait_bytes(ref, sem):
    pltpu.make_async_copy(ref, ref, sem).wait()


def weights_kernel(
    n_gr,
    n_fs,
    n_tp,
    gu,
    dn,
    tok,
    gu_out,
    dn_out,
    tok_out,
    gu_recv,
    dn_recv,
    send_sems,
    relay_send,
    relay_recv,
    tok_recv,
    own_sems,
):
    experts = n_fs * n_tp
    my_gr = lax.axis_index("gr")
    me = lax.axis_index("fs") * n_tp + lax.axis_index("tp")
    greet(me, experts, n_tp, my_gr, n_gr)
    own = (
        pltpu.make_async_copy(gu.at[me], gu_out.at[my_gr, me], own_sems.at[0]),
        pltpu.make_async_copy(dn.at[me], dn_out.at[my_gr, me], own_sems.at[1]),
        pltpu.make_async_copy(tok.at[me], tok_out.at[me], tok_recv),
    )
    for copy in own:
        copy.start()

    def start_weights(step, carry):
        to = lax.rem(me + step, experts)
        where = place(to, n_tp)
        send(gu.at[to], gu_out.at[my_gr, me], send_sems.at[0], gu_recv.at[me], where).start()
        send(dn.at[to], dn_out.at[my_gr, me], send_sems.at[1], dn_recv.at[me], where).start()
        return carry

    lax.fori_loop(1, experts, start_weights, 0)

    def start_tokens(step, carry):
        to = lax.rem(me + step, experts)
        send(tok.at[to], tok_out.at[me], send_sems.at[2], tok_recv, place(to, n_tp)).start()
        return carry

    lax.fori_loop(1, experts, start_tokens, 0)

    def relay(gu_from, dn_from, source):
        for step in range(1, n_gr):
            other = lax.rem(my_gr + step, n_gr)
            where = {"gr": other}
            send(
                gu_from,
                gu_out.at[my_gr, source],
                relay_send.at[0, step],
                relay_recv.at[0, step],
                where,
            ).start()
            send(
                dn_from,
                dn_out.at[my_gr, source],
                relay_send.at[1, step],
                relay_recv.at[1, step],
                where,
            ).start()

    relay(gu.at[me], dn.at[me], me)

    def arrive(step, carry):
        source = lax.rem(me + experts - step, experts)
        where = place(source, n_tp)
        landed_gu = gu_out.at[my_gr, source]
        landed_dn = dn_out.at[my_gr, source]
        send(landed_gu, landed_gu, send_sems.at[0], gu_recv.at[source], where).wait_recv()
        send(landed_dn, landed_dn, send_sems.at[1], dn_recv.at[source], where).wait_recv()
        relay(landed_gu, landed_dn, source)
        return carry

    lax.fori_loop(1, experts, arrive, 0)
    own[0].wait()
    own[1].wait()
    rest = pl.ds(0, experts - 1)
    wait_bytes(gu.at[rest], send_sems.at[0])
    wait_bytes(dn.at[rest], send_sems.at[1])
    wait_bytes(tok.at[rest], send_sems.at[2])
    wait_bytes(tok, tok_recv)
    for step in range(1, n_gr):
        wait_bytes(gu, relay_send.at[0, step])
        wait_bytes(dn, relay_send.at[1, step])
        wait_bytes(gu, relay_recv.at[0, step])
        wait_bytes(dn, relay_recv.at[1, step])


def return_kernel(n_gr, n_fs, n_tp, rows, rows_out, send_sem, recv_sem):
    experts = n_fs * n_tp
    me = lax.axis_index("fs") * n_tp + lax.axis_index("tp")
    greet(me, experts, n_tp, 0, 1)
    pltpu.make_async_copy(rows.at[me], rows_out.at[me], recv_sem).start()

    def start(step, carry):
        to = lax.rem(me + step, experts)
        send(rows.at[to], rows_out.at[me], send_sem, recv_sem, place(to, n_tp)).start()
        return carry

    lax.fori_loop(1, experts, start, 0)
    wait_bytes(rows.at[pl.ds(0, experts - 1)], send_sem)
    wait_bytes(rows, recv_sem)


def body(
    tokens, norm_gain, gate_master, up_master, down_master, route_group, route_expert, route_weight
):
    n_fs = lax.axis_size("fs")
    n_tp = lax.axis_size("tp")
    n_gr = lax.axis_size("gr")
    experts = n_fs * n_tp
    per_group = experts // E_GROUPS
    d_local, f_local = gate_master.shape[1:]
    gate_cast = (gate_master * norm_gain[None, :, None]).astype(jnp.bfloat16)
    up_cast = (up_master * norm_gain[None, :, None]).astype(jnp.bfloat16)
    gu = jnp.concatenate([jnp.swapaxes(gate_cast, 1, 2), jnp.swapaxes(up_cast, 1, 2)], axis=1)
    dn = down_master.astype(jnp.bfloat16)

    count, width = tokens.shape
    floats = tokens.astype(jnp.float32)
    normed = (floats * lax.rsqrt(jnp.mean(floats * floats, axis=-1, keepdims=True) + 1e-06)).astype(
        jnp.bfloat16
    )
    capacity = 3 * count * TOP // (2 * experts)
    pairs = count * TOP
    flat_ids = (route_group[:, None] * per_group + route_expert).reshape(-1)
    columns = lax.broadcasted_iota(jnp.int32, (pairs, experts), 1)
    chosen = flat_ids[:, None] == columns
    earlier = lax.broadcasted_iota(jnp.int32, (pairs, pairs), 1) < lax.broadcasted_iota(
        jnp.int32, (pairs, pairs), 0
    )
    before = jnp.dot(
        earlier.astype(jnp.bfloat16),
        chosen.astype(jnp.bfloat16),
        preferred_element_type=jnp.float32,
    )
    rank = jnp.sum(jnp.where(chosen, before, 0.0), axis=1).astype(jnp.int32)
    dump = experts * capacity
    slot = jnp.where(rank < capacity, flat_ids * capacity + rank, dump).reshape(count, TOP)
    slots = lax.broadcasted_iota(jnp.int32, (count, dump), 1)
    picks = [(slot[:, k][:, None] == slots).astype(jnp.bfloat16) for k in range(TOP)]
    outgoing = lax.dot_general(
        sum(picks[1:], picks[0]),
        normed,
        (((0,), (0,)), ((), ())),
        preferred_element_type=jnp.float32,
    ).astype(jnp.bfloat16)
    outgoing = outgoing.reshape(experts, capacity, width)

    def shape(*dims):
        return jax.ShapeDtypeStruct(dims, jnp.bfloat16)

    dma = pltpu.SemaphoreType.DMA
    gu_all, dn_all, block = pl.pallas_call(
        functools.partial(weights_kernel, n_gr, n_fs, n_tp),
        name="handover",
        out_shape=(shape(n_gr, *gu.shape), shape(n_gr, *dn.shape), shape(*outgoing.shape)),
        in_specs=[ANY] * 3,
        out_specs=(ANY,) * 3,
        scratch_shapes=[
            dma((experts,)),
            dma((experts,)),
            dma((3,)),
            dma((2, n_gr)),
            dma((2, n_gr)),
            dma,
            dma((2,)),
        ],
        compiler_params=pltpu.CompilerParams(collective_id=0, has_side_effects=True),
    )(gu, dn, outgoing)

    tiles = gu_all.reshape(n_gr, n_fs, n_tp, 2, f_local, d_local)
    gate_up = jnp.transpose(tiles, (3, 1, 5, 0, 2, 4)).reshape(
        2, 1, n_fs * d_local, n_gr * n_tp * f_local
    )
    gate_new, up_new = gate_up[0], gate_up[1]
    fz, dw = dn.shape[1:]
    down_new = jnp.transpose(dn_all.reshape(n_gr, n_fs, n_tp, fz, dw), (1, 3, 0, 2, 4)).reshape(
        1, n_fs * fz, n_gr * n_tp * dw
    )

    flat_rows = block.reshape(-1, width)
    gate = jnp.dot(flat_rows, gate_new[0], preferred_element_type=jnp.float32)
    upper = jnp.dot(flat_rows, up_new[0], preferred_element_type=jnp.float32)
    hidden = (jax.nn.silu(gate) * upper).astype(jnp.bfloat16)
    result = jnp.dot(hidden, down_new[0], preferred_element_type=jnp.float32).astype(jnp.bfloat16)
    returned = pl.pallas_call(
        functools.partial(return_kernel, n_gr, n_fs, n_tp),
        name="give_back",
        out_shape=shape(*block.shape),
        in_specs=[ANY],
        out_specs=ANY,
        scratch_shapes=[dma, dma],
        compiler_params=pltpu.CompilerParams(collective_id=1, has_side_effects=True),
    )(result.reshape(block.shape))
    table = returned.reshape(dump, width)
    mixed = sum(
        jnp.dot(picks[k], table, preferred_element_type=jnp.float32) * route_weight[:, k][:, None]
        for k in range(TOP)
    ).astype(jnp.bfloat16)
    return (gate_new, up_new, down_new, mixed)


def solution(mesh):
    placed = (
        P(("gr", "fs", "tp"), None),
        P("fs"),
        P(None, "fs", ("gr", "tp")),
        P(None, "fs", ("gr", "tp")),
        P(None, "fs", ("gr", "tp")),
        P(("gr", "fs", "tp")),
        P(("gr", "fs", "tp"), None),
        P(("gr", "fs", "tp"), None),
    )
    return jax.shard_map(
        body,
        mesh=mesh,
        in_specs=placed,
        out_specs=(
            P(("fs", "tp"), None, None),
            P(("fs", "tp"), None, None),
            P(("fs", "tp"), None, None),
            P(("gr", "fs", "tp"), None),
        ),
        check_vma=False,
    )
```

```python
import functools

import jax
import jax.numpy as jnp
from jax import lax
from jax.experimental import pallas as pl
from jax.experimental.pallas import tpu as pltpu
from jax.sharding import PartitionSpec as P

E_GROUPS = 4
TOP = 2
MESH = pl.DeviceIdType.MESH
ANY = pl.BlockSpec(memory_space=pl.ANY)


def place(expert, n_tp):
    return {"fs": expert // n_tp, "tp": lax.rem(expert, n_tp)}


def greet(me, experts, n_tp, my_gr, n_gr):
    barrier = pltpu.get_barrier_semaphore()

    def hello(step, carry):
        pl.semaphore_signal(
            barrier,
            inc=1,
            device_id=place(lax.rem(me + step, experts), n_tp),
            device_id_type=MESH,
        )
        return carry

    lax.fori_loop(1, experts, hello, 0)
    for step in range(1, n_gr):
        pl.semaphore_signal(
            barrier, inc=1, device_id={"gr": lax.rem(my_gr + step, n_gr)}, device_id_type=MESH
        )
    pl.semaphore_wait(barrier, experts - 1 + n_gr - 1)


def send(src, dst, send_sem, recv_sem, where):
    return pltpu.make_async_remote_copy(
        src_ref=src,
        dst_ref=dst,
        send_sem=send_sem,
        recv_sem=recv_sem,
        device_id=where,
        device_id_type=MESH,
    )


def wait_bytes(ref, sem):
    pltpu.make_async_copy(ref, ref, sem).wait()


def fused_kernel(
    n_gr,
    n_fs,
    n_tp,
    gu,
    dn,
    tok,
    gu_full,
    dn_full,
    returned,
    gu_land,
    dn_land,
    tok_land,
    result,
    gu_whole,
    dn_whole,
    gu_recv,
    dn_recv,
    tok_recv,
    send_sems,
    relay_send,
    relay_recv,
    ret_recv,
    own_sems,
    out_sems,
):
    experts = n_fs * n_tp
    my_gr = lax.axis_index("gr")
    my_fs = lax.axis_index("fs")
    my_tp = lax.axis_index("tp")
    me = my_fs * n_tp + my_tp
    f_two, d_local = gu.shape[1:]
    f_local = f_two // 2
    fz, dw = dn.shape[1:]
    units = n_gr * n_tp * f_local

    def target(step):
        return lax.rem(my_fs + step // n_tp, n_fs) * n_tp + lax.rem(my_tp + step, n_tp)

    def origin(step):
        return lax.rem(my_fs + n_fs - step // n_tp, n_fs) * n_tp + lax.rem(
            my_tp + n_tp - lax.rem(step, n_tp), n_tp
        )

    greet(me, experts, n_tp, my_gr, n_gr)
    own = (
        pltpu.make_async_copy(gu.at[me], gu_land.at[my_gr, me], own_sems.at[0]),
        pltpu.make_async_copy(dn.at[me], dn_land.at[my_gr, me], own_sems.at[1]),
        pltpu.make_async_copy(tok.at[me], tok_land.at[me], tok_recv.at[me]),
    )
    for copy in own:
        copy.start()

    def start_weights(step, carry):
        to = target(step)
        where = place(to, n_tp)
        send(gu.at[to], gu_land.at[my_gr, me], send_sems.at[0], gu_recv.at[me], where).start()
        send(dn.at[to], dn_land.at[my_gr, me], send_sems.at[1], dn_recv.at[me], where).start()
        return carry

    lax.fori_loop(1, experts, start_weights, 0)

    def start_tokens(step, carry):
        to = target(step)
        send(
            tok.at[to], tok_land.at[me], send_sems.at[2], tok_recv.at[me], place(to, n_tp)
        ).start()
        return carry

    lax.fori_loop(1, experts, start_tokens, 0)

    def relay(gu_from, dn_from, source):
        for step in range(1, n_gr):
            where = {"gr": lax.rem(my_gr + step, n_gr)}
            send(
                gu_from,
                gu_land.at[my_gr, source],
                relay_send.at[0, step],
                relay_recv.at[0, step],
                where,
            ).start()
            send(
                dn_from,
                dn_land.at[my_gr, source],
                relay_send.at[1, step],
                relay_recv.at[1, step],
                where,
            ).start()

    relay(gu.at[me], dn.at[me], me)

    def arrive(step, carry):
        source = origin(step)
        where = place(source, n_tp)
        landed_gu = gu_land.at[my_gr, source]
        landed_dn = dn_land.at[my_gr, source]
        send(landed_gu, landed_gu, send_sems.at[0], gu_recv.at[source], where).wait_recv()
        send(landed_dn, landed_dn, send_sems.at[1], dn_recv.at[source], where).wait_recv()
        relay(landed_gu, landed_dn, source)
        return carry

    lax.fori_loop(1, experts, arrive, 0)
    own[0].wait()
    own[1].wait()
    for step in range(1, n_gr):
        wait_bytes(gu, relay_recv.at[0, step])
        wait_bytes(dn, relay_recv.at[1, step])

    def assemble(part, carry):
        g = part // n_tp
        t = lax.rem(part, n_tp)
        rows = pl.multiple_of(part * f_local, f_local)
        cols = pl.multiple_of(part * dw, dw)
        for z in range(n_fs):
            tile = gu_land[g, z * n_tp + t]
            width = pl.ds(z * d_local, d_local)
            gu_whole[pl.ds(rows, f_local), width] = tile[:f_local]
            gu_whole[pl.ds(units + rows, f_local), width] = tile[f_local:]
            dn_whole[pl.ds(z * fz, fz), pl.ds(cols, dw)] = dn_land[g, z * n_tp + t]
        return carry

    lax.fori_loop(0, n_gr * n_tp, assemble, 0)

    def give(step):
        source = origin(step)
        send(
            result.at[source], returned.at[me], send_sems.at[3], ret_recv, place(source, n_tp)
        ).start()

    def work(step, carry):
        source = origin(step)
        landed = tok_land.at[source]
        pltpu.make_async_copy(landed, landed, tok_recv.at[source]).wait()
        both = lax.dot_general(
            tok_land[source],
            gu_whole[...],
            (((1,), (1,)), ((), ())),
            preferred_element_type=jnp.float32,
        )
        gate, upper = both[:, :units], both[:, units:]
        hidden = (gate / (1.0 + jnp.exp(-gate)) * upper).astype(jnp.bfloat16)
        result[source] = jnp.dot(
            hidden, dn_whole[...], preferred_element_type=jnp.float32
        ).astype(jnp.bfloat16)

        @pl.when(step > 1)
        def _():
            give(step - 1)

        return carry

    lax.fori_loop(0, experts, work, 0)
    give(experts - 1)
    kept = pltpu.make_async_copy(result.at[me], returned.at[me], ret_recv)
    kept.start()
    outs = (
        pltpu.make_async_copy(gu_whole, gu_full, out_sems.at[0]),
        pltpu.make_async_copy(dn_whole, dn_full, out_sems.at[1]),
    )
    for copy in outs:
        copy.start()
    rest = pl.ds(0, experts - 1)
    wait_bytes(gu.at[rest], send_sems.at[0])
    wait_bytes(dn.at[rest], send_sems.at[1])
    wait_bytes(tok.at[rest], send_sems.at[2])
    for step in range(1, n_gr):
        wait_bytes(gu, relay_send.at[0, step])
        wait_bytes(dn, relay_send.at[1, step])
    for copy in outs:
        copy.wait()
    wait_bytes(tok.at[rest], send_sems.at[3])
    wait_bytes(tok, ret_recv)


def body(
    tokens, norm_gain, gate_master, up_master, down_master, route_group, route_expert, route_weight
):
    n_fs = lax.axis_size("fs")
    n_tp = lax.axis_size("tp")
    n_gr = lax.axis_size("gr")
    experts = n_fs * n_tp
    per_group = experts // E_GROUPS
    d_local, f_local = gate_master.shape[1:]
    gate_cast = (gate_master * norm_gain[None, :, None]).astype(jnp.bfloat16)
    up_cast = (up_master * norm_gain[None, :, None]).astype(jnp.bfloat16)
    gu = jnp.concatenate([jnp.swapaxes(gate_cast, 1, 2), jnp.swapaxes(up_cast, 1, 2)], axis=1)
    dn = down_master.astype(jnp.bfloat16)

    count, width = tokens.shape
    floats = tokens.astype(jnp.float32)
    normed = (floats * lax.rsqrt(jnp.mean(floats * floats, axis=-1, keepdims=True) + 1e-06)).astype(
        jnp.bfloat16
    )
    capacity = 3 * count * TOP // (2 * experts)
    pairs = count * TOP
    flat_ids = (route_group[:, None] * per_group + route_expert).reshape(-1)
    columns = lax.broadcasted_iota(jnp.int32, (pairs, experts), 1)
    chosen = flat_ids[:, None] == columns
    earlier = lax.broadcasted_iota(jnp.int32, (pairs, pairs), 1) < lax.broadcasted_iota(
        jnp.int32, (pairs, pairs), 0
    )
    before = jnp.dot(
        earlier.astype(jnp.bfloat16),
        chosen.astype(jnp.bfloat16),
        preferred_element_type=jnp.float32,
    )
    rank = jnp.sum(jnp.where(chosen, before, 0.0), axis=1).astype(jnp.int32)
    dump = experts * capacity
    slot = jnp.where(rank < capacity, flat_ids * capacity + rank, dump).reshape(count, TOP)
    slots = lax.broadcasted_iota(jnp.int32, (count, dump), 1)
    picks = [(slot[:, k][:, None] == slots).astype(jnp.bfloat16) for k in range(TOP)]
    outgoing = lax.dot_general(
        sum(picks[1:], picks[0]),
        normed,
        (((0,), (0,)), ((), ())),
        preferred_element_type=jnp.float32,
    ).astype(jnp.bfloat16)
    outgoing = outgoing.reshape(experts, capacity, width)

    def shape(*dims):
        return jax.ShapeDtypeStruct(dims, jnp.bfloat16)

    dma = pltpu.SemaphoreType.DMA
    vmem = functools.partial(pltpu.VMEM, dtype=jnp.bfloat16)
    units = n_gr * n_tp * f_local
    full = (2 * units, n_fs * d_local)
    down_full = (n_fs * dn.shape[1], n_gr * n_tp * dn.shape[2])
    gu_full, dn_full, returned = pl.pallas_call(
        functools.partial(fused_kernel, n_gr, n_fs, n_tp),
        name="experts",
        out_shape=(shape(*full), shape(*down_full), shape(*outgoing.shape)),
        in_specs=[ANY] * 3,
        out_specs=(ANY,) * 3,
        scratch_shapes=[
            vmem((n_gr, *gu.shape)),
            vmem((n_gr, *dn.shape)),
            vmem(outgoing.shape),
            vmem(outgoing.shape),
            vmem(full),
            vmem(down_full),
            dma((experts,)),
            dma((experts,)),
            dma((experts,)),
            dma((4,)),
            dma((2, n_gr)),
            dma((2, n_gr)),
            dma,
            dma((2,)),
            dma((2,)),
        ],
        compiler_params=pltpu.CompilerParams(collective_id=0, has_side_effects=True),
    )(gu, dn, outgoing)
    gate_new = jnp.swapaxes(gu_full[:units], 0, 1)[None]
    up_new = jnp.swapaxes(gu_full[units:], 0, 1)[None]
    down_new = dn_full[None]
    table = returned.reshape(dump, width)
    mixed = sum(
        jnp.dot(picks[k], table, preferred_element_type=jnp.float32) * route_weight[:, k][:, None]
        for k in range(TOP)
    ).astype(jnp.bfloat16)
    return (gate_new, up_new, down_new, mixed)


def solution(mesh):
    placed = (
        P(("gr", "fs", "tp"), None),
        P("fs"),
        P(None, "fs", ("gr", "tp")),
        P(None, "fs", ("gr", "tp")),
        P(None, "fs", ("gr", "tp")),
        P(("gr", "fs", "tp")),
        P(("gr", "fs", "tp"), None),
        P(("gr", "fs", "tp"), None),
    )
    return jax.shard_map(
        body,
        mesh=mesh,
        in_specs=placed,
        out_specs=(
            P(("fs", "tp"), None, None),
            P(("fs", "tp"), None, None),
            P(("fs", "tp"), None, None),
            P(("gr", "fs", "tp"), None),
        ),
        check_vma=False,
    )
```

```python
import functools

import jax
import jax.numpy as jnp
from jax import lax
from jax.experimental import pallas as pl
from jax.experimental.pallas import tpu as pltpu
from jax.sharding import PartitionSpec as P

E_GROUPS = 4
TOP = 2
MESH = pl.DeviceIdType.MESH
ANY = pl.BlockSpec(memory_space=pl.ANY)


def place(expert, n_tp):
    return {"fs": expert // n_tp, "tp": lax.rem(expert, n_tp)}


def greet(me, experts, n_tp, my_gr, n_gr):
    barrier = pltpu.get_barrier_semaphore()

    def hello(step, carry):
        pl.semaphore_signal(
            barrier,
            inc=1,
            device_id=place(lax.rem(me + step, experts), n_tp),
            device_id_type=MESH,
        )
        return carry

    lax.fori_loop(1, experts, hello, 0)
    for step in range(1, n_gr):
        pl.semaphore_signal(
            barrier, inc=1, device_id={"gr": lax.rem(my_gr + step, n_gr)}, device_id_type=MESH
        )
    pl.semaphore_wait(barrier, experts - 1 + n_gr - 1)


def send(src, dst, send_sem, recv_sem, where):
    return pltpu.make_async_remote_copy(
        src_ref=src,
        dst_ref=dst,
        send_sem=send_sem,
        recv_sem=recv_sem,
        device_id=where,
        device_id_type=MESH,
    )


def wait_bytes(ref, sem):
    pltpu.make_async_copy(ref, ref, sem).wait()


def fused_kernel(
    n_gr,
    n_fs,
    n_tp,
    gu,
    dn,
    tok,
    gu_full,
    dn_full,
    returned,
    gu_land,
    dn_land,
    tok_land,
    result,
    gu_whole,
    dn_whole,
    gu_recv,
    dn_recv,
    tok_recv,
    send_sems,
    relay_send,
    relay_recv,
    ret_recv,
    own_sems,
    out_sems,
):
    experts = n_fs * n_tp
    my_gr = lax.axis_index("gr")
    my_fs = lax.axis_index("fs")
    my_tp = lax.axis_index("tp")
    me = my_fs * n_tp + my_tp
    f_two, d_local = gu.shape[1:]
    f_local = f_two // 2
    fz, dw = dn.shape[1:]
    units = n_gr * n_tp * f_local

    def target(step):
        return lax.rem(my_fs + step // n_tp, n_fs) * n_tp + lax.rem(my_tp + step, n_tp)

    def origin(step):
        return lax.rem(my_fs + n_fs - step // n_tp, n_fs) * n_tp + lax.rem(
            my_tp + n_tp - lax.rem(step, n_tp), n_tp
        )

    greet(me, experts, n_tp, my_gr, n_gr)
    own = (
        pltpu.make_async_copy(gu.at[me], gu_land.at[my_gr, me], own_sems.at[0]),
        pltpu.make_async_copy(dn.at[me], dn_land.at[my_gr, me], own_sems.at[1]),
        pltpu.make_async_copy(tok.at[me], tok_land.at[me], tok_recv.at[me]),
    )
    for copy in own:
        copy.start()

    def start_weights(step, carry):
        to = target(step)
        where = place(to, n_tp)
        send(gu.at[to], gu_land.at[my_gr, me], send_sems.at[0], gu_recv.at[me], where).start()
        send(dn.at[to], dn_land.at[my_gr, me], send_sems.at[1], dn_recv.at[me], where).start()
        return carry

    lax.fori_loop(1, experts, start_weights, 0)

    def start_tokens(step, carry):
        to = target(step)
        send(
            tok.at[to], tok_land.at[me], send_sems.at[2], tok_recv.at[me], place(to, n_tp)
        ).start()
        return carry

    lax.fori_loop(1, experts, start_tokens, 0)

    def relay(gu_from, dn_from, source):
        for step in range(1, n_gr):
            where = {"gr": lax.rem(my_gr + step, n_gr)}
            send(
                gu_from,
                gu_land.at[my_gr, source],
                relay_send.at[0, step],
                relay_recv.at[0, step],
                where,
            ).start()
            send(
                dn_from,
                dn_land.at[my_gr, source],
                relay_send.at[1, step],
                relay_recv.at[1, step],
                where,
            ).start()

    relay(gu.at[me], dn.at[me], me)

    def arrive(step, carry):
        source = origin(step)
        where = place(source, n_tp)
        landed_gu = gu_land.at[my_gr, source]
        landed_dn = dn_land.at[my_gr, source]
        send(landed_gu, landed_gu, send_sems.at[0], gu_recv.at[source], where).wait_recv()
        send(landed_dn, landed_dn, send_sems.at[1], dn_recv.at[source], where).wait_recv()
        relay(landed_gu, landed_dn, source)
        return carry

    lax.fori_loop(1, experts, arrive, 0)
    own[0].wait()
    own[1].wait()
    for step in range(1, n_gr):
        wait_bytes(gu, relay_recv.at[0, step])
        wait_bytes(dn, relay_recv.at[1, step])

    def assemble(part, carry):
        g = part // n_tp
        t = lax.rem(part, n_tp)
        rows = pl.multiple_of(part * f_local, f_local)
        cols = pl.multiple_of(part * dw, dw)
        for z in range(n_fs):
            tile = gu_land[g, z * n_tp + t]
            width = pl.ds(z * d_local, d_local)
            gu_whole[pl.ds(rows, f_local), width] = tile[:f_local]
            gu_whole[pl.ds(units + rows, f_local), width] = tile[f_local:]
            dn_whole[pl.ds(z * fz, fz), pl.ds(cols, dw)] = dn_land[g, z * n_tp + t]
        return carry

    lax.fori_loop(0, n_gr * n_tp, assemble, 0)

    def give(step):
        source = origin(step)
        send(
            result.at[source], returned.at[me], send_sems.at[3], ret_recv, place(source, n_tp)
        ).start()

    def work(step, carry):
        source = origin(step)
        landed = tok_land.at[source]
        pltpu.make_async_copy(landed, landed, tok_recv.at[source]).wait()
        both = lax.dot_general(
            tok_land[source],
            gu_whole[...],
            (((1,), (1,)), ((), ())),
            preferred_element_type=jnp.float32,
        )
        gate, upper = both[:, :units], both[:, units:]
        hidden = (gate / (1.0 + jnp.exp(-gate)) * upper).astype(jnp.bfloat16)
        result[source] = jnp.dot(
            hidden, dn_whole[...], preferred_element_type=jnp.float32
        ).astype(jnp.bfloat16)

        @pl.when(step > 1)
        def _():
            give(step - 1)

        return carry

    lax.fori_loop(0, experts, work, 0)
    give(experts - 1)
    kept = pltpu.make_async_copy(result.at[me], returned.at[me], ret_recv)
    kept.start()
    outs = (
        pltpu.make_async_copy(gu_whole, gu_full, out_sems.at[0]),
        pltpu.make_async_copy(dn_whole, dn_full, out_sems.at[1]),
    )
    for copy in outs:
        copy.start()
    rest = pl.ds(0, experts - 1)
    wait_bytes(gu.at[rest], send_sems.at[0])
    wait_bytes(dn.at[rest], send_sems.at[1])
    wait_bytes(tok.at[rest], send_sems.at[2])
    for step in range(1, n_gr):
        wait_bytes(gu, relay_send.at[0, step])
        wait_bytes(dn, relay_send.at[1, step])
    for copy in outs:
        copy.wait()
    wait_bytes(tok.at[rest], send_sems.at[3])
    wait_bytes(tok, ret_recv)


def plane_kernel(
    n_gr,
    n_fs,
    n_tp,
    gu,
    dn,
    rows,
    facts,
    gu_full,
    dn_full,
    returned,
    gu_land,
    dn_land,
    row_land,
    fact_land,
    block_out,
    block_land,
    result_out,
    result_land,
    mix_out,
    gu_whole,
    dn_whole,
    gu_recv,
    dn_recv,
    row_recv,
    fact_recv,
    block_recv,
    result_recv,
    send_sems,
    relay_send,
    relay_recv,
    ret_recv,
    own_sems,
    out_sems,
):
    experts = n_fs * n_tp
    my_gr = lax.axis_index("gr")
    my_fs = lax.axis_index("fs")
    my_tp = lax.axis_index("tp")
    me = my_fs * n_tp + my_tp
    f_two, d_local = gu.shape[1:]
    f_local = f_two // 2
    fz, dw = dn.shape[1:]
    units = n_gr * n_tp * f_local
    count = rows.shape[1]
    capacity = block_land.shape[2]

    def target(step):
        return lax.rem(my_fs + step // n_tp, n_fs) * n_tp + lax.rem(my_tp + step, n_tp)

    def origin(step):
        return lax.rem(my_fs + n_fs - step // n_tp, n_fs) * n_tp + lax.rem(
            my_tp + n_tp - lax.rem(step, n_tp), n_tp
        )

    greet(me, experts, n_tp, my_gr, n_gr)
    own = (
        pltpu.make_async_copy(gu.at[me], gu_land.at[my_gr, me], own_sems.at[0]),
        pltpu.make_async_copy(dn.at[me], dn_land.at[my_gr, me], own_sems.at[1]),
        pltpu.make_async_copy(rows.at[my_fs], row_land.at[my_fs], row_recv.at[my_fs]),
        pltpu.make_async_copy(facts.at[my_fs], fact_land.at[my_fs], fact_recv.at[my_fs]),
    )
    for copy in own:
        copy.start()

    def start_weights(step, carry):
        to = target(step)
        where = place(to, n_tp)
        send(gu.at[to], gu_land.at[my_gr, me], send_sems.at[0], gu_recv.at[me], where).start()
        send(dn.at[to], dn_land.at[my_gr, me], send_sems.at[1], dn_recv.at[me], where).start()
        return carry

    lax.fori_loop(1, experts, start_weights, 0)

    def start_rows(step, carry):
        to = lax.rem(my_fs + step, n_fs)
        where = {"fs": to}
        send(facts.at[to], fact_land.at[my_fs], send_sems.at[3], fact_recv.at[my_fs], where).start()
        send(rows.at[to], row_land.at[my_fs], send_sems.at[2], row_recv.at[my_fs], where).start()
        return carry

    lax.fori_loop(1, n_fs, start_rows, 0)

    def relay(gu_from, dn_from, source):
        for step in range(1, n_gr):
            where = {"gr": lax.rem(my_gr + step, n_gr)}
            send(
                gu_from,
                gu_land.at[my_gr, source],
                relay_send.at[0, step],
                relay_recv.at[0, step],
                where,
            ).start()
            send(
                dn_from,
                dn_land.at[my_gr, source],
                relay_send.at[1, step],
                relay_recv.at[1, step],
                where,
            ).start()

    relay(gu.at[me], dn.at[me], me)

    def arrive(step, carry):
        source = origin(step)
        where = place(source, n_tp)
        landed_gu = gu_land.at[my_gr, source]
        landed_dn = dn_land.at[my_gr, source]
        send(landed_gu, landed_gu, send_sems.at[0], gu_recv.at[source], where).wait_recv()
        send(landed_dn, landed_dn, send_sems.at[1], dn_recv.at[source], where).wait_recv()
        relay(landed_gu, landed_dn, source)
        return carry

    lax.fori_loop(1, experts, arrive, 0)
    own[0].wait()
    own[1].wait()
    for step in range(1, n_gr):
        wait_bytes(gu, relay_recv.at[0, step])
        wait_bytes(dn, relay_recv.at[1, step])

    def assemble(part, carry):
        g = part // n_tp
        t = lax.rem(part, n_tp)
        rows = pl.multiple_of(part * f_local, f_local)
        cols = pl.multiple_of(part * dw, dw)
        for z in range(n_fs):
            tile = gu_land[g, z * n_tp + t]
            width = pl.ds(z * d_local, d_local)
            gu_whole[pl.ds(rows, f_local), width] = tile[:f_local]
            gu_whole[pl.ds(units + rows, f_local), width] = tile[f_local:]
            dn_whole[pl.ds(z * fz, fz), pl.ds(cols, dw)] = dn_land[g, z * n_tp + t]
        return carry

    lax.fori_loop(0, n_gr * n_tp, assemble, 0)

    def plane_of(step):
        return lax.rem(my_fs + n_fs - step, n_fs)

    def wait_for(ref, sem):
        pltpu.make_async_copy(ref, ref, sem).wait()

    def hand_out(step):
        plane = plane_of(step)
        wait_for(fact_land.at[plane], fact_recv.at[plane])
        wait_for(row_land.at[plane], row_recv.at[plane])
        fact = fact_land[plane]
        spots = lax.broadcasted_iota(jnp.int32, (capacity, count), 0).astype(jnp.float32) + 1.0
        block = row_land[plane]
        for turn in list(range(1, n_tp)) + [0]:
            to = lax.rem(my_tp + turn, n_tp)
            wanted = spots + (to * capacity).astype(jnp.float32)
            hit = wanted == fact[0:1, :count]
            for k in range(1, TOP):
                hit = jnp.logical_or(hit, wanted == fact[k : k + 1, :count])
            taken = jnp.dot(
                jnp.where(hit, 1.0, 0.0).astype(jnp.bfloat16),
                block,
                preferred_element_type=jnp.float32,
            ).astype(jnp.bfloat16)
            if turn:
                block_out[plane, turn - 1] = taken
            else:
                block_land[plane, my_tp] = taken
        for turn in range(1, n_tp):
            send(
                block_out.at[plane, turn - 1],
                block_land.at[plane, my_tp],
                send_sems.at[4],
                block_recv.at[plane, my_tp],
                {"tp": lax.rem(my_tp + turn, n_tp)},
            ).start()

    def work(step):
        plane = plane_of(step)

        def give(turn):
            send(
                result_out.at[plane, turn - 1],
                result_land.at[plane, my_tp],
                send_sems.at[5],
                result_recv.at[plane],
                {"tp": lax.rem(my_tp + n_tp - turn, n_tp)},
            ).start()

        for turn in list(range(1, n_tp)) + [0]:
            source = lax.rem(my_tp + n_tp - turn, n_tp)
            if turn:
                wait_for(block_land.at[plane, source], block_recv.at[plane, source])
            both = lax.dot_general(
                block_land[plane, source],
                gu_whole[...],
                (((1,), (1,)), ((), ())),
                preferred_element_type=jnp.float32,
            )
            gate, upper = both[:, :units], both[:, units:]
            hidden = (gate / (1.0 + jnp.exp(-gate)) * upper).astype(jnp.bfloat16)
            done = jnp.dot(hidden, dn_whole[...], preferred_element_type=jnp.float32).astype(
                jnp.bfloat16
            )
            if turn:
                result_out[plane, turn - 1] = done
            else:
                result_land[plane, my_tp] = done
            if turn > 1:
                give(turn - 1)
        give(n_tp - 1)

    def mix(step):
        plane = plane_of(step)
        wait_for(result_out.at[plane], result_recv.at[plane])
        fact = jnp.transpose(fact_land[plane])[:count]
        total = None
        for k in range(TOP):
            picked = None
            for t in range(n_tp):
                spots = lax.broadcasted_iota(jnp.int32, (count, capacity), 1) + (1 + t * capacity)
                hit = spots.astype(jnp.float32) == fact[:, k : k + 1]
                term = jnp.dot(
                    jnp.where(hit, 1.0, 0.0).astype(jnp.bfloat16),
                    result_land[plane, t],
                    preferred_element_type=jnp.float32,
                )
                picked = term if picked is None else picked + term
            part = picked * fact[:, TOP + k : TOP + k + 1]
            total = part if total is None else total + part
        mix_out[plane] = total.astype(jnp.bfloat16)

    def send_mix(step):
        plane = plane_of(step)
        send(
            mix_out.at[plane], returned.at[my_fs], send_sems.at[6], ret_recv, {"fs": plane}
        ).start()

    def pipeline(step, carry):
        @pl.when(step >= 2)
        def _():
            mix(step - 2)

        @pl.when(step < n_fs)
        def _():
            hand_out(step)

        @pl.when(step > 2)
        def _():
            send_mix(step - 2)

        @pl.when(jnp.logical_and(step >= 1, step <= n_fs))
        def _():
            work(step - 1)

        return carry

    lax.fori_loop(0, n_fs + 2, pipeline, 0)
    pltpu.make_async_copy(mix_out.at[my_fs], returned.at[my_fs], ret_recv).start()
    outs = (
        pltpu.make_async_copy(gu_whole, gu_full, out_sems.at[0]),
        pltpu.make_async_copy(dn_whole, dn_full, out_sems.at[1]),
    )
    for copy in outs:
        copy.start()
    rest = pl.ds(0, experts - 1)
    others = pl.ds(0, n_fs - 1)
    wait_bytes(gu.at[rest], send_sems.at[0])
    wait_bytes(dn.at[rest], send_sems.at[1])
    wait_bytes(rows.at[others], send_sems.at[2])
    wait_bytes(facts.at[others], send_sems.at[3])
    wait_bytes(block_out, send_sems.at[4])
    wait_bytes(result_out, send_sems.at[5])
    for step in range(1, n_gr):
        wait_bytes(gu, relay_send.at[0, step])
        wait_bytes(dn, relay_send.at[1, step])
    for copy in outs:
        copy.wait()
    wait_bytes(mix_out.at[others], send_sems.at[6])
    wait_bytes(mix_out, ret_recv)


def body(
    tokens, norm_gain, gate_master, up_master, down_master, route_group, route_expert, route_weight
):
    n_fs = lax.axis_size("fs")
    n_tp = lax.axis_size("tp")
    n_gr = lax.axis_size("gr")
    experts = n_fs * n_tp
    per_group = experts // E_GROUPS
    d_local, f_local = gate_master.shape[1:]
    gate_cast = (gate_master * norm_gain[None, :, None]).astype(jnp.bfloat16)
    up_cast = (up_master * norm_gain[None, :, None]).astype(jnp.bfloat16)
    gu = jnp.concatenate([jnp.swapaxes(gate_cast, 1, 2), jnp.swapaxes(up_cast, 1, 2)], axis=1)
    dn = down_master.astype(jnp.bfloat16)

    count, width = tokens.shape
    floats = tokens.astype(jnp.float32)
    normed = (floats * lax.rsqrt(jnp.mean(floats * floats, axis=-1, keepdims=True) + 1e-06)).astype(
        jnp.bfloat16
    )
    capacity = 3 * count * TOP // (2 * experts)
    pairs = count * TOP
    flat_ids = (route_group[:, None] * per_group + route_expert).reshape(-1)
    columns = lax.broadcasted_iota(jnp.int32, (pairs, experts), 1)
    chosen = flat_ids[:, None] == columns
    earlier = lax.broadcasted_iota(jnp.int32, (pairs, pairs), 1) < lax.broadcasted_iota(
        jnp.int32, (pairs, pairs), 0
    )
    before = jnp.dot(
        earlier.astype(jnp.bfloat16),
        chosen.astype(jnp.bfloat16),
        preferred_element_type=jnp.float32,
    )
    rank = jnp.sum(jnp.where(chosen, before, 0.0), axis=1).astype(jnp.int32)
    dump = experts * capacity
    slot = jnp.where(rank < capacity, flat_ids * capacity + rank, dump).reshape(count, TOP)
    def shape(*dims):
        return jax.ShapeDtypeStruct(dims, jnp.bfloat16)

    dma = pltpu.SemaphoreType.DMA
    vmem = functools.partial(pltpu.VMEM, dtype=jnp.bfloat16)
    units = n_gr * n_tp * f_local
    full = (2 * units, n_fs * d_local)
    down_full = (n_fs * dn.shape[1], n_gr * n_tp * dn.shape[2])
    if per_group == n_tp and TOP == 2:
        kept = rank.reshape(count, TOP) < capacity
        held = jnp.any(kept, axis=1)
        most = min(count, capacity * (n_tp - 1))
        ahead = (
            (route_group[:, None] == route_group[None, :])
            & held[None, :]
            & (
                lax.broadcasted_iota(jnp.int32, (count, count), 1)
                < lax.broadcasted_iota(jnp.int32, (count, count), 0)
            )
        )
        spot = jnp.sum(ahead.astype(jnp.int32), axis=1)
        row = jnp.where(held, route_group * most + spot, n_fs * most)
        lies = row[:, None] == lax.broadcasted_iota(jnp.int32, (count, n_fs * most), 1)
        picks = lies.astype(jnp.bfloat16)
        outgoing = lax.dot_general(
            picks, normed, (((0,), (0,)), ((), ())), preferred_element_type=jnp.float32
        ).astype(jnp.bfloat16)
        outgoing = outgoing.reshape(n_fs, most, width)
        inside = jnp.where(kept, route_expert * capacity + rank.reshape(count, TOP) + 1, 0)
        values = [inside[:, k].astype(jnp.float32) for k in range(TOP)]
        values += [route_weight[:, k] for k in range(TOP)]
        facts = jnp.stack(
            [jnp.sum(jnp.where(lies, v[:, None], 0.0), axis=0).reshape(n_fs, most) for v in values],
            axis=1,
        )
        lanes = -(-most // 128) * 128
        facts = jnp.pad(facts, ((0, 0), (0, 8 - 2 * TOP), (0, lanes - most)))
        blocks = (n_fs, n_tp, capacity, width)
        fewer = (n_fs, n_tp - 1, capacity, width)
        gu_full, dn_full, returned = pl.pallas_call(
            functools.partial(plane_kernel, n_gr, n_fs, n_tp),
            name="planes",
            out_shape=(shape(*full), shape(*down_full), shape(*outgoing.shape)),
            in_specs=[ANY] * 4,
            out_specs=(ANY,) * 3,
            scratch_shapes=[
                vmem((n_gr, *gu.shape)),
                vmem((n_gr, *dn.shape)),
                vmem(outgoing.shape),
                pltpu.VMEM(facts.shape, jnp.float32),
                vmem(fewer),
                vmem(blocks),
                vmem(fewer),
                vmem(blocks),
                vmem(outgoing.shape),
                vmem(full),
                vmem(down_full),
                dma((experts,)),
                dma((experts,)),
                dma((n_fs,)),
                dma((n_fs,)),
                dma((n_fs, n_tp)),
                dma((n_fs,)),
                dma((7,)),
                dma((2, n_gr)),
                dma((2, n_gr)),
                dma,
                dma((2,)),
                dma((2,)),
            ],
            compiler_params=pltpu.CompilerParams(collective_id=0, has_side_effects=True),
        )(gu, dn, outgoing, facts)
        mixed = jnp.dot(
            picks, returned.reshape(-1, width), preferred_element_type=jnp.float32
        ).astype(jnp.bfloat16)
    else:
        slots = lax.broadcasted_iota(jnp.int32, (count, dump), 1)
        picks = [(slot[:, k][:, None] == slots).astype(jnp.bfloat16) for k in range(TOP)]
        outgoing = lax.dot_general(
            sum(picks[1:], picks[0]),
            normed,
            (((0,), (0,)), ((), ())),
            preferred_element_type=jnp.float32,
        ).astype(jnp.bfloat16)
        outgoing = outgoing.reshape(experts, capacity, width)

        gu_full, dn_full, returned = pl.pallas_call(
            functools.partial(fused_kernel, n_gr, n_fs, n_tp),
            name="experts",
            out_shape=(shape(*full), shape(*down_full), shape(*outgoing.shape)),
            in_specs=[ANY] * 3,
            out_specs=(ANY,) * 3,
            scratch_shapes=[
                vmem((n_gr, *gu.shape)),
                vmem((n_gr, *dn.shape)),
                vmem(outgoing.shape),
                vmem(outgoing.shape),
                vmem(full),
                vmem(down_full),
                dma((experts,)),
                dma((experts,)),
                dma((experts,)),
                dma((4,)),
                dma((2, n_gr)),
                dma((2, n_gr)),
                dma,
                dma((2,)),
                dma((2,)),
            ],
            compiler_params=pltpu.CompilerParams(collective_id=0, has_side_effects=True),
        )(gu, dn, outgoing)
        table = returned.reshape(dump, width)
        mixed = sum(
            jnp.dot(picks[k], table, preferred_element_type=jnp.float32) * route_weight[:, k][:, None]
            for k in range(TOP)
        ).astype(jnp.bfloat16)
    gate_new = jnp.swapaxes(gu_full[:units], 0, 1)[None]
    up_new = jnp.swapaxes(gu_full[units:], 0, 1)[None]
    down_new = dn_full[None]
    return (gate_new, up_new, down_new, mixed)


def solution(mesh):
    placed = (
        P(("gr", "fs", "tp"), None),
        P("fs"),
        P(None, "fs", ("gr", "tp")),
        P(None, "fs", ("gr", "tp")),
        P(None, "fs", ("gr", "tp")),
        P(("gr", "fs", "tp")),
        P(("gr", "fs", "tp"), None),
        P(("gr", "fs", "tp"), None),
    )
    return jax.shard_map(
        body,
        mesh=mesh,
        in_specs=placed,
        out_specs=(
            P(("fs", "tp"), None, None),
            P(("fs", "tp"), None, None),
            P(("fs", "tp"), None, None),
            P(("gr", "fs", "tp"), None),
        ),
        check_vma=False,
    )
```

```python
import functools

import jax
import jax.numpy as jnp
from jax import lax
from jax.experimental import pallas as pl
from jax.experimental.pallas import tpu as pltpu
from jax.sharding import PartitionSpec as P

E_GROUPS = 4
TOP = 2
MESH = pl.DeviceIdType.MESH
ANY = pl.BlockSpec(memory_space=pl.ANY)


def place(expert, n_tp):
    return {"fs": expert // n_tp, "tp": lax.rem(expert, n_tp)}


def greet(me, experts, n_tp, my_gr, n_gr):
    barrier = pltpu.get_barrier_semaphore()

    def hello(step, carry):
        pl.semaphore_signal(
            barrier,
            inc=1,
            device_id=place(lax.rem(me + step, experts), n_tp),
            device_id_type=MESH,
        )
        return carry

    lax.fori_loop(1, experts, hello, 0)
    for step in range(1, n_gr):
        pl.semaphore_signal(
            barrier, inc=1, device_id={"gr": lax.rem(my_gr + step, n_gr)}, device_id_type=MESH
        )
    pl.semaphore_wait(barrier, experts - 1 + n_gr - 1)


def send(src, dst, send_sem, recv_sem, where):
    return pltpu.make_async_remote_copy(
        src_ref=src,
        dst_ref=dst,
        send_sem=send_sem,
        recv_sem=recv_sem,
        device_id=where,
        device_id_type=MESH,
    )


def wait_bytes(ref, sem):
    pltpu.make_async_copy(ref, ref, sem).wait()


def fused_kernel(
    n_gr,
    n_fs,
    n_tp,
    gu,
    dn,
    tok,
    gu_full,
    dn_full,
    returned,
    gu_land,
    dn_land,
    tok_land,
    result,
    gu_whole,
    dn_whole,
    gu_recv,
    dn_recv,
    tok_recv,
    send_sems,
    relay_send,
    relay_recv,
    ret_recv,
    own_sems,
    out_sems,
):
    experts = n_fs * n_tp
    my_gr = lax.axis_index("gr")
    my_fs = lax.axis_index("fs")
    my_tp = lax.axis_index("tp")
    me = my_fs * n_tp + my_tp
    f_two, d_local = gu.shape[1:]
    f_local = f_two // 2
    fz, dw = dn.shape[1:]
    units = n_gr * n_tp * f_local

    def target(step):
        return lax.rem(my_fs + step // n_tp, n_fs) * n_tp + lax.rem(my_tp + step, n_tp)

    def origin(step):
        return lax.rem(my_fs + n_fs - step // n_tp, n_fs) * n_tp + lax.rem(
            my_tp + n_tp - lax.rem(step, n_tp), n_tp
        )

    greet(me, experts, n_tp, my_gr, n_gr)
    own = (
        pltpu.make_async_copy(gu.at[me], gu_land.at[my_gr, me], own_sems.at[0]),
        pltpu.make_async_copy(dn.at[me], dn_land.at[my_gr, me], own_sems.at[1]),
        pltpu.make_async_copy(tok.at[me], tok_land.at[me], tok_recv.at[me]),
    )
    for copy in own:
        copy.start()

    def start_weights(step, carry):
        to = target(step)
        where = place(to, n_tp)
        send(gu.at[to], gu_land.at[my_gr, me], send_sems.at[0], gu_recv.at[me], where).start()
        send(dn.at[to], dn_land.at[my_gr, me], send_sems.at[1], dn_recv.at[me], where).start()
        return carry

    lax.fori_loop(1, experts, start_weights, 0)

    def start_tokens(step, carry):
        to = target(step)
        send(
            tok.at[to], tok_land.at[me], send_sems.at[2], tok_recv.at[me], place(to, n_tp)
        ).start()
        return carry

    lax.fori_loop(1, experts, start_tokens, 0)

    def relay(gu_from, dn_from, source):
        for step in range(1, n_gr):
            where = {"gr": lax.rem(my_gr + step, n_gr)}
            send(
                gu_from,
                gu_land.at[my_gr, source],
                relay_send.at[0, step],
                relay_recv.at[0, step],
                where,
            ).start()
            send(
                dn_from,
                dn_land.at[my_gr, source],
                relay_send.at[1, step],
                relay_recv.at[1, step],
                where,
            ).start()

    relay(gu.at[me], dn.at[me], me)

    def arrive(step, carry):
        source = origin(step)
        where = place(source, n_tp)
        landed_gu = gu_land.at[my_gr, source]
        landed_dn = dn_land.at[my_gr, source]
        send(landed_gu, landed_gu, send_sems.at[0], gu_recv.at[source], where).wait_recv()
        send(landed_dn, landed_dn, send_sems.at[1], dn_recv.at[source], where).wait_recv()
        relay(landed_gu, landed_dn, source)
        return carry

    lax.fori_loop(1, experts, arrive, 0)
    own[0].wait()
    own[1].wait()
    for step in range(1, n_gr):
        wait_bytes(gu, relay_recv.at[0, step])
        wait_bytes(dn, relay_recv.at[1, step])

    def assemble(part, carry):
        g = part // n_tp
        t = lax.rem(part, n_tp)
        rows = pl.multiple_of(part * f_local, f_local)
        cols = pl.multiple_of(part * dw, dw)
        for z in range(n_fs):
            tile = gu_land[g, z * n_tp + t]
            width = pl.ds(z * d_local, d_local)
            gu_whole[pl.ds(rows, f_local), width] = tile[:f_local]
            gu_whole[pl.ds(units + rows, f_local), width] = tile[f_local:]
            dn_whole[pl.ds(z * fz, fz), pl.ds(cols, dw)] = dn_land[g, z * n_tp + t]
        return carry

    lax.fori_loop(0, n_gr * n_tp, assemble, 0)

    def give(step):
        source = origin(step)
        send(
            result.at[source], returned.at[me], send_sems.at[3], ret_recv, place(source, n_tp)
        ).start()

    def work(step, carry):
        source = origin(step)
        landed = tok_land.at[source]
        pltpu.make_async_copy(landed, landed, tok_recv.at[source]).wait()
        both = lax.dot_general(
            tok_land[source],
            gu_whole[...],
            (((1,), (1,)), ((), ())),
            preferred_element_type=jnp.float32,
        )
        gate, upper = both[:, :units], both[:, units:]
        hidden = (gate / (1.0 + jnp.exp(-gate)) * upper).astype(jnp.bfloat16)
        result[source] = jnp.dot(
            hidden, dn_whole[...], preferred_element_type=jnp.float32
        ).astype(jnp.bfloat16)

        @pl.when(step > 1)
        def _():
            give(step - 1)

        return carry

    lax.fori_loop(0, experts, work, 0)
    give(experts - 1)
    kept = pltpu.make_async_copy(result.at[me], returned.at[me], ret_recv)
    kept.start()
    outs = (
        pltpu.make_async_copy(gu_whole, gu_full, out_sems.at[0]),
        pltpu.make_async_copy(dn_whole, dn_full, out_sems.at[1]),
    )
    for copy in outs:
        copy.start()
    rest = pl.ds(0, experts - 1)
    wait_bytes(gu.at[rest], send_sems.at[0])
    wait_bytes(dn.at[rest], send_sems.at[1])
    wait_bytes(tok.at[rest], send_sems.at[2])
    for step in range(1, n_gr):
        wait_bytes(gu, relay_send.at[0, step])
        wait_bytes(dn, relay_send.at[1, step])
    for copy in outs:
        copy.wait()
    wait_bytes(tok.at[rest], send_sems.at[3])
    wait_bytes(tok, ret_recv)


def plane_kernel(
    n_gr,
    n_fs,
    n_tp,
    gu,
    dn,
    rows,
    facts,
    gu_full,
    dn_full,
    returned,
    gu_land,
    dn_land,
    row_land,
    fact_land,
    block_out,
    block_land,
    result_out,
    result_land,
    mix_out,
    gu_whole,
    dn_whole,
    gu_recv,
    dn_recv,
    row_recv,
    fact_recv,
    block_recv,
    result_recv,
    send_sems,
    relay_send,
    relay_recv,
    ret_recv,
    own_sems,
    out_sems,
):
    experts = n_fs * n_tp
    my_gr = lax.axis_index("gr")
    my_fs = lax.axis_index("fs")
    my_tp = lax.axis_index("tp")
    me = my_fs * n_tp + my_tp
    f_two, d_local = gu.shape[1:]
    f_local = f_two // 2
    fz, dw = dn.shape[1:]
    units = n_gr * n_tp * f_local
    count = rows.shape[1]
    capacity = block_land.shape[2]

    def target(step):
        return lax.rem(my_fs + step // n_tp, n_fs) * n_tp + lax.rem(my_tp + step, n_tp)

    def origin(step):
        return lax.rem(my_fs + n_fs - step // n_tp, n_fs) * n_tp + lax.rem(
            my_tp + n_tp - lax.rem(step, n_tp), n_tp
        )

    greet(me, experts, n_tp, my_gr, n_gr)
    own = (
        pltpu.make_async_copy(gu.at[me], gu_land.at[my_gr, me], own_sems.at[0]),
        pltpu.make_async_copy(dn.at[me], dn_land.at[my_gr, me], own_sems.at[1]),
        pltpu.make_async_copy(rows.at[my_fs], row_land.at[my_fs], row_recv.at[my_fs]),
        pltpu.make_async_copy(facts.at[my_fs], fact_land.at[my_fs], fact_recv.at[my_fs]),
    )
    for copy in own:
        copy.start()

    def start_weights(step, carry):
        to = target(step)
        where = place(to, n_tp)
        send(gu.at[to], gu_land.at[my_gr, me], send_sems.at[0], gu_recv.at[me], where).start()
        send(dn.at[to], dn_land.at[my_gr, me], send_sems.at[1], dn_recv.at[me], where).start()
        return carry

    lax.fori_loop(1, experts, start_weights, 0)

    def start_rows(step, carry):
        to = lax.rem(my_fs + step, n_fs)
        where = {"fs": to}
        send(facts.at[to], fact_land.at[my_fs], send_sems.at[3], fact_recv.at[my_fs], where).start()
        send(rows.at[to], row_land.at[my_fs], send_sems.at[2], row_recv.at[my_fs], where).start()
        return carry

    lax.fori_loop(1, n_fs, start_rows, 0)

    def relay(gu_from, dn_from, source):
        for step in range(1, n_gr):
            where = {"gr": lax.rem(my_gr + step, n_gr)}
            send(
                gu_from,
                gu_land.at[my_gr, source],
                relay_send.at[0, step],
                relay_recv.at[0, step],
                where,
            ).start()
            send(
                dn_from,
                dn_land.at[my_gr, source],
                relay_send.at[1, step],
                relay_recv.at[1, step],
                where,
            ).start()

    relay(gu.at[me], dn.at[me], me)

    def arrive(step, carry):
        source = origin(step)
        where = place(source, n_tp)
        landed_gu = gu_land.at[my_gr, source]
        landed_dn = dn_land.at[my_gr, source]
        send(landed_gu, landed_gu, send_sems.at[0], gu_recv.at[source], where).wait_recv()
        send(landed_dn, landed_dn, send_sems.at[1], dn_recv.at[source], where).wait_recv()
        relay(landed_gu, landed_dn, source)
        return carry

    lax.fori_loop(1, experts, arrive, 0)
    own[0].wait()
    own[1].wait()
    for step in range(1, n_gr):
        wait_bytes(gu, relay_recv.at[0, step])
        wait_bytes(dn, relay_recv.at[1, step])

    def assemble(part, carry):
        g = part // n_tp
        t = lax.rem(part, n_tp)
        rows = pl.multiple_of(part * f_local, f_local)
        cols = pl.multiple_of(part * dw, dw)
        for z in range(n_fs):
            tile = gu_land[g, z * n_tp + t]
            width = pl.ds(z * d_local, d_local)
            gu_whole[pl.ds(rows, f_local), width] = tile[:f_local]
            gu_whole[pl.ds(units + rows, f_local), width] = tile[f_local:]
            dn_whole[pl.ds(z * fz, fz), pl.ds(cols, dw)] = dn_land[g, z * n_tp + t]
        return carry

    lax.fori_loop(0, n_gr * n_tp, assemble, 0)

    def plane_of(step):
        return lax.rem(my_fs + n_fs - step, n_fs)

    def wait_for(ref, sem):
        pltpu.make_async_copy(ref, ref, sem).wait()

    def join(blocks):
        wide = blocks.astype(jnp.float32)
        return wide.reshape(n_tp * capacity, wide.shape[2]).astype(jnp.bfloat16)

    def split(wide):
        return wide.reshape(n_tp, capacity, wide.shape[1]).astype(jnp.bfloat16)

    def hand_out(step):
        plane = plane_of(step)
        wait_for(fact_land.at[plane], fact_recv.at[plane])
        wait_for(row_land.at[plane], row_recv.at[plane])
        fact = fact_land[plane]
        spots = lax.broadcasted_iota(jnp.int32, (n_tp * capacity, count), 0).astype(jnp.float32)
        spots = spots + 1.0
        hit = spots == fact[0:1, :count]
        for k in range(1, TOP):
            hit = jnp.logical_or(hit, spots == fact[k : k + 1, :count])
        taken = jnp.dot(
            jnp.where(hit, 1.0, 0.0).astype(jnp.bfloat16),
            row_land[plane],
            preferred_element_type=jnp.float32,
        )
        block_out[plane] = split(taken)
        block_land[plane, my_tp] = block_out[plane, my_tp]
        for turn in range(1, n_tp):
            to = lax.rem(my_tp + turn, n_tp)
            send(
                block_out.at[plane, to],
                block_land.at[plane, my_tp],
                send_sems.at[4],
                block_recv.at[plane, my_tp],
                {"tp": to},
            ).start()

    def work(step):
        plane = plane_of(step)
        for turn in range(1, n_tp):
            source = lax.rem(my_tp + n_tp - turn, n_tp)
            wait_for(block_land.at[plane, source], block_recv.at[plane, source])
        both = lax.dot_general(
            join(block_land[plane]),
            gu_whole[...],
            (((1,), (1,)), ((), ())),
            preferred_element_type=jnp.float32,
        )
        gate, upper = both[:, :units], both[:, units:]
        hidden = (gate / (1.0 + jnp.exp(-gate)) * upper).astype(jnp.bfloat16)
        done = jnp.dot(hidden, dn_whole[...], preferred_element_type=jnp.float32)
        result_out[plane] = split(done)
        result_land[plane, my_tp] = result_out[plane, my_tp]
        for turn in range(1, n_tp):
            source = lax.rem(my_tp + n_tp - turn, n_tp)
            send(
                result_out.at[plane, source],
                result_land.at[plane, my_tp],
                send_sems.at[5],
                result_recv.at[plane],
                {"tp": source},
            ).start()

    def mix(step):
        plane = plane_of(step)
        wait_for(result_out.at[plane, pl.ds(0, n_tp - 1)], result_recv.at[plane])
        fact = jnp.transpose(fact_land[plane])[:count]
        found = join(result_land[plane])
        spots = lax.broadcasted_iota(jnp.int32, (count, n_tp * capacity), 1) + 1
        spots = spots.astype(jnp.float32)
        total = None
        for k in range(TOP):
            picked = jnp.dot(
                jnp.where(spots == fact[:, k : k + 1], 1.0, 0.0).astype(jnp.bfloat16),
                found,
                preferred_element_type=jnp.float32,
            )
            part = picked * fact[:, TOP + k : TOP + k + 1]
            total = part if total is None else total + part
        mix_out[plane] = total.astype(jnp.bfloat16)

    def send_mix(step):
        plane = plane_of(step)
        send(
            mix_out.at[plane], returned.at[my_fs], send_sems.at[6], ret_recv, {"fs": plane}
        ).start()

    def pipeline(step, carry):
        @pl.when(step >= 2)
        def _():
            mix(step - 2)

        @pl.when(step < n_fs)
        def _():
            hand_out(step)

        @pl.when(step > 2)
        def _():
            send_mix(step - 2)

        @pl.when(jnp.logical_and(step >= 1, step <= n_fs))
        def _():
            work(step - 1)

        return carry

    lax.fori_loop(0, n_fs + 2, pipeline, 0)
    pltpu.make_async_copy(mix_out.at[my_fs], returned.at[my_fs], ret_recv).start()
    outs = (
        pltpu.make_async_copy(gu_whole, gu_full, out_sems.at[0]),
        pltpu.make_async_copy(dn_whole, dn_full, out_sems.at[1]),
    )
    for copy in outs:
        copy.start()
    rest = pl.ds(0, experts - 1)
    others = pl.ds(0, n_fs - 1)
    wait_bytes(gu.at[rest], send_sems.at[0])
    wait_bytes(dn.at[rest], send_sems.at[1])
    wait_bytes(rows.at[others], send_sems.at[2])
    wait_bytes(facts.at[others], send_sems.at[3])
    sent = block_out.at[:, pl.ds(0, n_tp - 1)]
    wait_bytes(sent, send_sems.at[4])
    wait_bytes(sent, send_sems.at[5])
    for step in range(1, n_gr):
        wait_bytes(gu, relay_send.at[0, step])
        wait_bytes(dn, relay_send.at[1, step])
    for copy in outs:
        copy.wait()
    wait_bytes(mix_out.at[others], send_sems.at[6])
    wait_bytes(mix_out, ret_recv)


def body(
    tokens, norm_gain, gate_master, up_master, down_master, route_group, route_expert, route_weight
):
    n_fs = lax.axis_size("fs")
    n_tp = lax.axis_size("tp")
    n_gr = lax.axis_size("gr")
    experts = n_fs * n_tp
    per_group = experts // E_GROUPS
    d_local, f_local = gate_master.shape[1:]
    gate_cast = (gate_master * norm_gain[None, :, None]).astype(jnp.bfloat16)
    up_cast = (up_master * norm_gain[None, :, None]).astype(jnp.bfloat16)
    gu = jnp.concatenate([jnp.swapaxes(gate_cast, 1, 2), jnp.swapaxes(up_cast, 1, 2)], axis=1)
    dn = down_master.astype(jnp.bfloat16)

    count, width = tokens.shape
    floats = tokens.astype(jnp.float32)
    normed = (floats * lax.rsqrt(jnp.mean(floats * floats, axis=-1, keepdims=True) + 1e-06)).astype(
        jnp.bfloat16
    )
    capacity = 3 * count * TOP // (2 * experts)
    pairs = count * TOP
    flat_ids = (route_group[:, None] * per_group + route_expert).reshape(-1)
    columns = lax.broadcasted_iota(jnp.int32, (pairs, experts), 1)
    chosen = flat_ids[:, None] == columns
    earlier = lax.broadcasted_iota(jnp.int32, (pairs, pairs), 1) < lax.broadcasted_iota(
        jnp.int32, (pairs, pairs), 0
    )
    before = jnp.dot(
        earlier.astype(jnp.bfloat16),
        chosen.astype(jnp.bfloat16),
        preferred_element_type=jnp.float32,
    )
    rank = jnp.sum(jnp.where(chosen, before, 0.0), axis=1).astype(jnp.int32)
    dump = experts * capacity
    slot = jnp.where(rank < capacity, flat_ids * capacity + rank, dump).reshape(count, TOP)
    def shape(*dims):
        return jax.ShapeDtypeStruct(dims, jnp.bfloat16)

    dma = pltpu.SemaphoreType.DMA
    vmem = functools.partial(pltpu.VMEM, dtype=jnp.bfloat16)
    units = n_gr * n_tp * f_local
    full = (2 * units, n_fs * d_local)
    down_full = (n_fs * dn.shape[1], n_gr * n_tp * dn.shape[2])
    if per_group == n_tp and TOP == 2:
        kept = rank.reshape(count, TOP) < capacity
        held = jnp.any(kept, axis=1)
        most = min(count, capacity * (n_tp - 1))
        ahead = (
            (route_group[:, None] == route_group[None, :])
            & held[None, :]
            & (
                lax.broadcasted_iota(jnp.int32, (count, count), 1)
                < lax.broadcasted_iota(jnp.int32, (count, count), 0)
            )
        )
        spot = jnp.sum(ahead.astype(jnp.int32), axis=1)
        row = jnp.where(held, route_group * most + spot, n_fs * most)
        lies = row[:, None] == lax.broadcasted_iota(jnp.int32, (count, n_fs * most), 1)
        picks = lies.astype(jnp.bfloat16)
        outgoing = lax.dot_general(
            picks, normed, (((0,), (0,)), ((), ())), preferred_element_type=jnp.float32
        ).astype(jnp.bfloat16)
        outgoing = outgoing.reshape(n_fs, most, width)
        inside = jnp.where(kept, route_expert * capacity + rank.reshape(count, TOP) + 1, 0)
        values = [inside[:, k].astype(jnp.float32) for k in range(TOP)]
        values += [route_weight[:, k] for k in range(TOP)]
        facts = jnp.stack(
            [jnp.sum(jnp.where(lies, v[:, None], 0.0), axis=0).reshape(n_fs, most) for v in values],
            axis=1,
        )
        lanes = -(-most // 128) * 128
        facts = jnp.pad(facts, ((0, 0), (0, 8 - 2 * TOP), (0, lanes - most)))
        blocks = (n_fs, n_tp, capacity, width)
        gu_full, dn_full, returned = pl.pallas_call(
            functools.partial(plane_kernel, n_gr, n_fs, n_tp),
            name="planes",
            out_shape=(shape(*full), shape(*down_full), shape(*outgoing.shape)),
            in_specs=[ANY] * 4,
            out_specs=(ANY,) * 3,
            scratch_shapes=[
                vmem((n_gr, *gu.shape)),
                vmem((n_gr, *dn.shape)),
                vmem(outgoing.shape),
                pltpu.VMEM(facts.shape, jnp.float32),
                vmem(blocks),
                vmem(blocks),
                vmem(blocks),
                vmem(blocks),
                vmem(outgoing.shape),
                vmem(full),
                vmem(down_full),
                dma((experts,)),
                dma((experts,)),
                dma((n_fs,)),
                dma((n_fs,)),
                dma((n_fs, n_tp)),
                dma((n_fs,)),
                dma((7,)),
                dma((2, n_gr)),
                dma((2, n_gr)),
                dma,
                dma((2,)),
                dma((2,)),
            ],
            compiler_params=pltpu.CompilerParams(collective_id=0, has_side_effects=True),
        )(gu, dn, outgoing, facts)
        mixed = jnp.dot(
            picks, returned.reshape(-1, width), preferred_element_type=jnp.float32
        ).astype(jnp.bfloat16)
    else:
        slots = lax.broadcasted_iota(jnp.int32, (count, dump), 1)
        picks = [(slot[:, k][:, None] == slots).astype(jnp.bfloat16) for k in range(TOP)]
        outgoing = lax.dot_general(
            sum(picks[1:], picks[0]),
            normed,
            (((0,), (0,)), ((), ())),
            preferred_element_type=jnp.float32,
        ).astype(jnp.bfloat16)
        outgoing = outgoing.reshape(experts, capacity, width)

        gu_full, dn_full, returned = pl.pallas_call(
            functools.partial(fused_kernel, n_gr, n_fs, n_tp),
            name="experts",
            out_shape=(shape(*full), shape(*down_full), shape(*outgoing.shape)),
            in_specs=[ANY] * 3,
            out_specs=(ANY,) * 3,
            scratch_shapes=[
                vmem((n_gr, *gu.shape)),
                vmem((n_gr, *dn.shape)),
                vmem(outgoing.shape),
                vmem(outgoing.shape),
                vmem(full),
                vmem(down_full),
                dma((experts,)),
                dma((experts,)),
                dma((experts,)),
                dma((4,)),
                dma((2, n_gr)),
                dma((2, n_gr)),
                dma,
                dma((2,)),
                dma((2,)),
            ],
            compiler_params=pltpu.CompilerParams(collective_id=0, has_side_effects=True),
        )(gu, dn, outgoing)
        table = returned.reshape(dump, width)
        mixed = sum(
            jnp.dot(picks[k], table, preferred_element_type=jnp.float32) * route_weight[:, k][:, None]
            for k in range(TOP)
        ).astype(jnp.bfloat16)
    gate_new = jnp.swapaxes(gu_full[:units], 0, 1)[None]
    up_new = jnp.swapaxes(gu_full[units:], 0, 1)[None]
    down_new = dn_full[None]
    return (gate_new, up_new, down_new, mixed)


def solution(mesh):
    placed = (
        P(("gr", "fs", "tp"), None),
        P("fs"),
        P(None, "fs", ("gr", "tp")),
        P(None, "fs", ("gr", "tp")),
        P(None, "fs", ("gr", "tp")),
        P(("gr", "fs", "tp")),
        P(("gr", "fs", "tp"), None),
        P(("gr", "fs", "tp"), None),
    )
    return jax.shard_map(
        body,
        mesh=mesh,
        in_specs=placed,
        out_specs=(
            P(("fs", "tp"), None, None),
            P(("fs", "tp"), None, None),
            P(("fs", "tp"), None, None),
            P(("gr", "fs", "tp"), None),
        ),
        check_vma=False,
    )
```
